32 devices in a mesh: ep: 32 (over z, y, x, core).
Axes of the slice: x: 2, y: 2, z: 4, core: 2. Of those that a mesh axis runs over, the one named last changes fastest.
Arguments:
- residual_in: bfloat16 [256, 2048], P('ep'), may hold values from -6 to 6
- gain_mix_pre: float32 [2048], replicated, may hold values from 0.1 to 1.9
- w_query: bfloat16 [2048, 2048], P(None, 'ep'), may hold values from -0.125 to 0.125
- w_key: bfloat16 [2048, 2048], P(None, 'ep'), may hold values from -0.125 to 0.125
- w_value: bfloat16 [2048, 2048], P(None, 'ep'), may hold values from -0.125 to 0.125
- w_outgate: bfloat16 [2048, 2048], P(None, 'ep'), may hold values from -0.125 to 0.125
- w_decay: bfloat16 [2048, 16], replicated, may hold values from -0.125 to 0.125
- w_beta: bfloat16 [2048, 16], replicated, may hold values from -0.125 to 0.125
- decay_scale: float32 [16], replicated, may hold values from 1 to 16
- decay_bias: float32 [16], replicated, may hold values from -5 to -1
- head_gain: float32 [128], replicated, may hold values from 0.1 to 1.9
- w_out: bfloat16 [2048, 2048], replicated, may hold values from -0.125 to 0.125
- gain_mix_post: float32 [2048], replicated, may hold values from 0.1 to 1.9
- state_cache: bfloat16 [256, 16, 128, 128], P('ep'), may hold values from -2.390625 to 2.390625
- gain_ffn_pre: float32 [2048], replicated, may hold values from 0.1 to 1.9
- routes: int32 [256, 4], P('ep'), may hold values from 0 to 7, all different within a row; in each aligned block of 8 rows (0 to 7, 8 to 15, ...) at most 8 rows name the same one
- route_logits: float32 [256, 4], P('ep'), may hold values from -6 to 6
- w_gate: bfloat16 [2048, 16384], P(None, 'ep'), may hold values from -0.375 to 0.375
- w_up: bfloat16 [2048, 16384], P(None, 'ep'), may hold values from -0.375 to 0.375
- w_down: bfloat16 [16384, 2048], P('ep'), may hold values from -0.125 to 0.125
- gain_ffn_post: float32 [2048], replicated, may hold values from 0.1 to 1.9
Outputs:
- result: bfloat16 [256, 2048], P('ep')
- new_state: bfloat16 [256, 16, 128, 128], P('ep')
The draws below stay inside these ranges and needn't reach their ends.
Inputs may be any that keep to these rules, and one draw needn't show every extreme that they name: `routes`: each row names 4 different experts. In the rows of one device (aligned blocks of 8 rows) no expert is named more than 8 times, and in some block one expert is named exactly 8 times.
All inputs are finite; a program needn't handle non-finite values.
Results may differ from the reference program's by a relative error of at most 0.014.
Values may be sent and summed in bfloat16 or wider, within the bound.
A program may use at most 128 MiB of HBM per device.

```python
import math
import jax
import jax.numpy as jnp
import numpy as np
from jax import lax

D = 2048
H = 16
HD = 128
FF = 2048
PIECES = 4
TOPK = 4
SEQ_DEV = 8
TOKENS = 256
EXPERTS = 8
CAP = 8
N_EP = 32


def level_of(own_key, shape, shards, low, top_value):
    def one(position, blocks):
        steps = jax.random.uniform(jax.random.fold_in(jax.random.fold_in(own_key, 6), position), (blocks,), jnp.float32, low / len(shards), top_value / len(shards))
        return jnp.repeat(jnp.exp(steps), shape[position] // blocks).reshape((-1,) + (1,) * (len(shape) - position - 1))

    gain = one(*shards[0])
    for cut in shards[1:]:
        gain = gain * one(*cut)
    return gain


def deal_out(stream_key, own, number, rows, count, top, limit, lean):
    ranking = jax.random.permutation(stream_key, count)
    heavy_load, common = shares(count, rows * top, limit, lean, True), shares(count, rows * top, limit, lean, False)
    places = jnp.arange(count)

    def named(sizes, rotation):
        used = int((sizes > 0).sum())
        fixed = max(1, used // 4)
        moved = fixed + (places - fixed + rotation * (used - fixed)) % max(1, count - fixed)
        return jnp.zeros((count,), jnp.int32).at[ranking[jnp.where(places < fixed, places, moved)]].set(jnp.asarray(sizes, jnp.int32))

    sizes = jnp.where(number % 4 == 0, named(heavy_load, number // 4), named(common, number - number // 4 - 1))
    mixed = jax.random.permutation(jax.random.fold_in(own, 3), count)
    source_of, receiver = mixed[0:count // 2 * 2:2], mixed[1:count // 2 * 2:2]
    room = jnp.minimum(sizes[source_of] - 1, limit - sizes[receiver]) // 2
    room = jnp.where((source_of == ranking[0]) | (receiver == ranking[0]) | (sizes[receiver] == 0), 0, jnp.maximum(room, 0))
    moved = jax.random.randint(jax.random.fold_in(own, 4), (count // 2,), 0, 1 << 20) % (room + 1)
    sizes = sizes.at[source_of].add(-moved).at[receiver].add(moved)
    members = jnp.searchsorted(jnp.cumsum(sizes), jnp.arange(rows * top), side="right").astype(jnp.int32)
    table = members.reshape(top, rows).T
    table = table[jax.random.permutation(jax.random.fold_in(own, 1), rows)]
    rotation = jax.random.randint(jax.random.fold_in(own, 2), (rows, 1), 0, top)
    return jnp.take_along_axis(table, (jnp.arange(top)[None, :] + rotation) % top, axis=1)


def shares(number_of, total, bound, slope, full):
    loads = [(1 << 20) // math.isqrt(standing ** slope) + 1 for standing in range(1, number_of + 1)]
    largest = bound if full else min(bound, max(-(-total // number_of), total * loads[0] // sum(loads)))
    least = 1 if total - largest >= number_of - 1 else 0
    holding, rest = [largest] + [least] * (number_of - 1), total - largest - least * (number_of - 1)
    while rest > 0:
        free = [i for i in range(1, number_of) if holding[i] < largest] or [i for i in range(1, number_of) if holding[i] < bound]
        mass, remaining = sum([loads[i] for i in free]), rest
        for i in free:
            more = min(bound - holding[i], max(1, remaining * loads[i] // mass), rest)
            holding[i] = holding[i] + more
            rest = rest - more
    return np.array(holding)


def noise(key, shape, scale, limit, pieces=(), held_as=jnp.bfloat16):
    values = scale * jax.random.normal(key, shape, jnp.float32)
    if pieces:
        values = values * level_of(key, shape, pieces, -0.22, 0.18)
    return jnp.clip(values, -limit, limit).astype(held_as)


def setup_inputs(seed: int = 0) -> dict:
    key_of = jax.random.split(jax.random.key(seed), 22)
    residual_in = noise(key_of[0], (TOKENS, D), 1.0, 6.0, ((0, 32),))
    gain_mix_pre = jnp.clip(1.0 + 0.18 * jax.random.normal(key_of[1], (D,), jnp.float32), 0.1, 1.9)
    w_query = noise(key_of[2], (D, H * HD), D ** -0.5, 0.125, ((1, 32),))
    w_key = noise(key_of[3], (D, H * HD), D ** -0.5, 0.125, ((1, 32),))
    w_value = noise(key_of[4], (D, H * HD), D ** -0.5, 0.125, ((1, 32),))
    w_outgate = noise(key_of[5], (D, H * HD), D ** -0.5, 0.125, ((1, 32),))
    w_decay = noise(key_of[6], (D, H), D ** -0.5, 0.125)
    w_beta = noise(key_of[7], (D, H), D ** -0.5, 0.125)
    decay_scale = jnp.clip(jnp.exp(jax.random.uniform(key_of[8], (H,), jnp.float32, math.log(1.0), math.log(16.0))), 1.0, 16.0)
    decay_bias = jnp.clip(jax.random.uniform(key_of[9], (H,), jnp.float32, -5.0, -1.0), -5.0, -1.0)
    head_gain = jnp.clip(1.0 + 0.18 * jax.random.normal(key_of[10], (HD,), jnp.float32), 0.1, 1.9)
    w_out = noise(key_of[11], (H * HD, D), (H * HD) ** -0.5, 0.125)
    gain_mix_post = jnp.clip(1.0 + 0.18 * jax.random.normal(key_of[12], (D,), jnp.float32), 0.1, 1.9)
    state_cache = noise(key_of[13], (TOKENS, H, HD, HD), 0.3, 2.390625, ((0, 32),))
    gain_ffn_pre = jnp.clip(1.0 + 0.18 * jax.random.normal(key_of[14], (D,), jnp.float32), 0.1, 1.9)
    routes_keys = jax.random.split(jax.random.fold_in(key_of[15], 1), TOKENS // SEQ_DEV)
    routes_turns = jax.random.permutation(jax.random.fold_in(key_of[15], 3), TOKENS // SEQ_DEV)
    routes = jax.vmap(lambda own, number: deal_out(jax.random.fold_in(key_of[15], 2), own, number, SEQ_DEV, EXPERTS, TOPK, CAP, 1))(routes_keys, routes_turns).reshape((TOKENS, TOPK))
    route_logits = noise(key_of[16], (TOKENS, TOPK), 1.0, 6.0, ((0, 32),), jnp.float32)
    w_gate = noise(key_of[17], (D, EXPERTS * FF), (D // 9) ** -0.5, 0.375, ((1, 32),))
    w_up = noise(key_of[18], (D, EXPERTS * FF), (D // 9) ** -0.5, 0.375, ((1, 32),))
    w_down = noise(key_of[19], (EXPERTS * FF, D), FF ** -0.5, 0.125, ((0, 32),))
    gain_ffn_post = jnp.clip(1.0 + 0.18 * jax.random.normal(key_of[20], (D,), jnp.float32), 0.1, 1.9)
    return dict(residual_in=residual_in, gain_mix_pre=gain_mix_pre, w_query=w_query, w_key=w_key, w_value=w_value, w_outgate=w_outgate, w_decay=w_decay, w_beta=w_beta, decay_scale=decay_scale, decay_bias=decay_bias, head_gain=head_gain, w_out=w_out, gain_mix_post=gain_mix_post, state_cache=state_cache, gain_ffn_pre=gain_ffn_pre, routes=routes, route_logits=route_logits, w_gate=w_gate, w_up=w_up, w_down=w_down, gain_ffn_post=gain_ffn_post)


EPS = 1e-06
LIMIT = 7.0
ALPHA = 1.702

def rms_scale(values):
    return values * lax.rsqrt(lax.optimization_barrier(jnp.mean(values * values, axis=-1, keepdims=True)) + EPS)

def clamped_unit(gate, upper):
    glu = jnp.minimum(gate, LIMIT)
    linear = jnp.clip(upper, -LIMIT, LIMIT)
    return glu * jax.nn.sigmoid(ALPHA * glu) * (linear + 1.0)

def dispatch_table(routes, experts, capacity):
    count, topk = routes.shape
    hits = (routes[:, :, None] == jnp.arange(experts, dtype=jnp.int32)).astype(jnp.int32)
    flat = hits.reshape(count * topk, experts)
    before = jnp.cumsum(flat, axis=0) - flat
    slots = lax.optimization_barrier(jnp.sum(before * flat, axis=1)).reshape(count, topk)
    target = routes * capacity + slots
    return (target[:, :, None] == jnp.arange(experts * capacity, dtype=jnp.int32)).astype(jnp.float32)

def delta_step(q_raw, k_raw, v_raw, z_raw, decay_in, beta_in, state, decay_scale, decay_bias, head_gain):
    count = q_raw.shape[0]
    query = jax.nn.silu(q_raw.astype(jnp.float32)).reshape(count, H, HD)
    query = query * lax.rsqrt(lax.optimization_barrier(jnp.sum(query * query, axis=-1, keepdims=True)) + EPS) * HD ** (-0.5)
    keys = jax.nn.silu(k_raw.astype(jnp.float32)).reshape(count, H, HD)
    keys = keys * lax.rsqrt(lax.optimization_barrier(jnp.sum(keys * keys, axis=-1, keepdims=True)) + EPS)
    values = jax.nn.silu(v_raw.astype(jnp.float32)).reshape(count, H, HD)
    decay = -decay_scale * jax.nn.softplus(decay_in + decay_bias)
    beta = jax.nn.sigmoid(beta_in)
    held = state.astype(jnp.float32) * jnp.exp(decay)[:, :, None, None]
    guess = jnp.einsum('rhk,rhkv->rhv', keys, held)
    held = held + jnp.einsum('rhk,rhv->rhkv', keys, beta[:, :, None] * (values - guess))
    output = jnp.einsum('rhk,rhkv->rhv', query, held)
    output = rms_scale(output) * head_gain
    gated = output.reshape(count, H * HD) * jax.nn.silu(z_raw.astype(jnp.float32))
    return (gated.astype(jnp.bfloat16), held.astype(jnp.bfloat16))

def reference(residual_in, gain_mix_pre, w_query, w_key, w_value, w_outgate, w_decay, w_beta, decay_scale, decay_bias, head_gain, w_out, gain_mix_post, state_cache, gain_ffn_pre, routes, route_logits, w_gate, w_up, w_down, gain_ffn_post):
    x_first = residual_in.astype(jnp.float32)
    normed = (rms_scale(x_first) * gain_mix_pre).astype(jnp.bfloat16)

    def project(weight):
        return jnp.dot(normed, weight, preferred_element_type=jnp.float32).astype(jnp.bfloat16)
    q_raw, k_raw, v_raw, z_raw = (project(w_query), project(w_key), project(w_value), project(w_outgate))
    decay_in = jnp.dot(normed, w_decay, preferred_element_type=jnp.float32)
    beta_in = jnp.dot(normed, w_beta, preferred_element_type=jnp.float32)

    def blocks(array):
        return array.reshape((N_EP, SEQ_DEV) + array.shape[1:])

    def block_step(items):
        return delta_step(*items, decay_scale, decay_bias, head_gain)
    mixed, new_state = lax.map(block_step, tuple((blocks(a) for a in (q_raw, k_raw, v_raw, z_raw, decay_in, beta_in, state_cache))))
    mixed = mixed.reshape(TOKENS, H * HD)
    new_state = new_state.reshape(TOKENS, H, HD, HD)
    branch = jnp.dot(mixed, w_out, preferred_element_type=jnp.float32)
    x_second = x_first + rms_scale(branch) * gain_mix_post
    normed_two = (rms_scale(x_second) * gain_ffn_pre).astype(jnp.bfloat16)
    table = jax.vmap(lambda r: dispatch_table(r, EXPERTS, CAP))(routes.reshape(N_EP, SEQ_DEV, TOPK))
    picks = lax.optimization_barrier(jnp.sum(table, axis=2))
    sent = jnp.einsum('nse,nsd->ned', picks, normed_two.reshape(N_EP, SEQ_DEV, D).astype(jnp.float32), precision=lax.Precision.HIGHEST).astype(jnp.bfloat16)
    sent = sent.reshape(N_EP, EXPERTS, CAP, D).transpose(1, 0, 2, 3).reshape(EXPERTS, N_EP * CAP, D)
    width = FF // PIECES

    def expert(items):
        rows_in, index = items
        total = jnp.zeros((N_EP * CAP, D), jnp.float32)
        for part in range(PIECES):
            start = (index * FF + part * width).astype(jnp.int32)
            gate_cols = lax.dynamic_slice_in_dim(w_gate, start, width, 1)
            up_cols = lax.dynamic_slice_in_dim(w_up, start, width, 1)
            down_rows = lax.dynamic_slice_in_dim(w_down, start, width, 0)
            hidden = clamped_unit(jnp.dot(rows_in, gate_cols, preferred_element_type=jnp.float32), jnp.dot(rows_in, up_cols, preferred_element_type=jnp.float32)).astype(jnp.bfloat16)
            piece_out = jnp.dot(hidden, down_rows, preferred_element_type=jnp.float32).astype(jnp.bfloat16)
            piece_out = lax.optimization_barrier(piece_out)
            total = total + piece_out.astype(jnp.float32)
        return total
    outputs = lax.map(expert, (sent, jnp.arange(EXPERTS, dtype=jnp.int32)))
    outputs = outputs.reshape(EXPERTS, N_EP, CAP, D).transpose(1, 0, 2, 3).reshape(N_EP, EXPERTS * CAP, D)
    raised = jnp.exp(route_logits)
    weights = raised / lax.optimization_barrier(jnp.sum(raised, axis=-1, keepdims=True))
    mix_table = jnp.einsum('nske,nsk->nse', table, weights.reshape(N_EP, SEQ_DEV, TOPK))
    moe = jnp.einsum('nse,ned->nsd', mix_table, outputs, precision=lax.Precision.HIGHEST).reshape(TOKENS, D)
    result = (x_second + rms_scale(moe) * gain_ffn_post).astype(jnp.bfloat16)
    return (result, new_state)
```

```python
import functools

import jax
import jax.numpy as jnp
from jax import lax
from jax.experimental import pallas as pl
from jax.experimental.pallas import tpu as pltpu
from jax.sharding import PartitionSpec as P

H = 16
HD = 128
PIECES = 4
TOPK = 4
LANES = 128
TAIL = 2 * LANES
MESH = pl.DeviceIdType.MESH

EPS = 1e-06
LIMIT = 7.0
ALPHA = 1.702


def rms_scale(values):
    return values * lax.rsqrt(jnp.mean(values * values, axis=-1, keepdims=True) + EPS)


def clamped_unit(gate, upper):
    glu = jnp.minimum(gate, LIMIT)
    linear = jnp.clip(upper, -LIMIT, LIMIT)
    return glu * jax.nn.sigmoid(ALPHA * glu) * (linear + 1.0)


def delta_step(
    q_raw, k_raw, v_raw, z_raw, decay_in, beta_in, state, decay_scale, decay_bias, head_gain
):
    count = q_raw.shape[0]
    query = jax.nn.silu(q_raw.astype(jnp.float32)).reshape(count, H, HD)
    query = query * lax.rsqrt(jnp.sum(query * query, axis=-1, keepdims=True) + EPS) * HD ** (-0.5)
    keys = jax.nn.silu(k_raw.astype(jnp.float32)).reshape(count, H, HD)
    keys = keys * lax.rsqrt(jnp.sum(keys * keys, axis=-1, keepdims=True) + EPS)
    values = jax.nn.silu(v_raw.astype(jnp.float32)).reshape(count, H, HD)
    decay = -decay_scale * jax.nn.softplus(decay_in + decay_bias)
    beta = jax.nn.sigmoid(beta_in)
    held = state.astype(jnp.float32) * jnp.exp(decay)[:, :, None, None]
    guess = jnp.einsum("rhk,rhkv->rhv", keys, held)
    held = held + jnp.einsum("rhk,rhv->rhkv", keys, beta[:, :, None] * (values - guess))
    output = jnp.einsum("rhk,rhkv->rhv", query, held)
    output = rms_scale(output) * head_gain
    gated = output.reshape(count, H * HD) * jax.nn.silu(z_raw.astype(jnp.float32))
    return (gated.astype(jnp.bfloat16), held.astype(jnp.bfloat16))

def flipped(value, distance):
    bit = 1
    while bit <= distance:
        if distance & bit:
            value = value + bit - 2 * bit * (lax.rem(value // bit, 2))
        bit *= 2
    return value


class Place:
    def __init__(self, devices):
        self.devices = devices
        self.layers = devices // 8
        self.me = lax.axis_index("ep")
        self.core = lax.rem(self.me, 2)
        self.x = lax.rem(self.me // 2, 2)
        self.y = lax.rem(self.me // 4, 2)
        self.z = self.me // 8

    def at(self, distance=0, y=0, x=0, core=0):
        z = flipped(self.z, distance)
        return (
            z * 8
            + flipped(self.y, y) * 4
            + flipped(self.x, x) * 2
            + flipped(self.core, core)
        )

    def partners(self):
        return [self.at(d) for d in range(1, self.layers)] + [
            self.at(y=1),
            self.at(x=1),
            self.at(core=1),
        ]


def greet(place):
    barrier = pltpu.get_barrier_semaphore()
    for partner in place.partners():
        pl.semaphore_signal(barrier, inc=1, device_id=(partner,), device_id_type=MESH)
    return lambda: pl.semaphore_wait(barrier, len(place.partners()))


def remote(source, target, send_sem, recv_sem, device):
    return pltpu.make_async_remote_copy(
        src_ref=source,
        dst_ref=target,
        send_sem=send_sem,
        recv_sem=recv_sem,
        device_id=(device,),
        device_id_type=MESH,
    )


def gather_sends(devices):
    layers = devices // 8
    return layers - 1 + 3 * layers + devices // 2


def gather_blocks(place, buf, send_sems, recv_sems):
    started = []

    def push(block, device):
        copy = remote(
            buf.at[block], buf.at[block], send_sems.at[len(started)], recv_sems.at[block], device
        )
        copy.start()
        started.append(copy)

    def arrive(block):
        remote(
            buf.at[block], buf.at[block], send_sems.at[0], recv_sems.at[block], place.at(core=1)
        ).wait_recv()

    def spread(distance):
        block = place.at(distance)
        push(block, place.at(x=1))
        push(block, place.at(y=1))
        push(block, place.at(core=1))

    def onward(distance):
        across_x, across_y = place.at(distance, x=1), place.at(distance, y=1)
        arrive(across_x)
        if distance % 2 == 0:
            push(across_x, place.at(y=1))
        push(across_x, place.at(core=1))
        arrive(across_y)
        if distance % 2 == 1:
            push(across_y, place.at(x=1))
        push(across_y, place.at(core=1))

    layers = place.layers
    for distance in range(layers - 1, 0, -1):
        push(place.me, place.at(distance))
    spread(0)
    for distance in range(1, layers):
        arrive(place.at(distance))
        spread(distance)
        onward(distance - 1)
    onward(layers - 1)
    for distance in range(layers):
        diagonal = place.at(distance, y=1, x=1)
        arrive(diagonal)
        push(diagonal, place.at(core=1))
    for distance in range(layers):
        for y in range(2):
            for x in range(2):
                arrive(place.at(distance, y, x, 1))
    return started


def settle(started):
    for copy in started:
        copy.wait_send()


def reduce_blocks(place, mine, paired, total, second, third, fourth, sems):
    pair_recv, send_sems, second_recv, third_recv, fourth_recv = sems
    started = []
    layers = place.layers

    def push(source, target, recv_sem, device):
        copy = remote(source, target, send_sems.at[len(started)], recv_sem, device)
        copy.start()
        started.append(copy)

    def arrive(target, recv_sem):
        remote(target, target, send_sems.at[0], recv_sem, place.at(core=1)).wait_recv()

    def wide(block):
        return block.astype(jnp.float32)

    order = list(range(layers - 1, -1, -1))
    for distance in order:
        for y, x in ((1, 1), (0, 1), (1, 0), (0, 0)):
            k = place.at(distance, y, x) // 2
            arrive(paired.at[k], pair_recv.at[k])
            total[k] = (wide(mine[k]) + wide(paired[k])).astype(jnp.bfloat16)
    for distance in order:
        if distance % 2 == 0:
            first, far, near = place.at(y=1), (1, 1), (1, 0)
        else:
            first, far, near = place.at(x=1), (1, 1), (0, 1)
        for slot, (y, x) in ((1, far), (0, near)):
            k = place.at(distance, y, x) // 2
            at = 2 * distance + slot
            push(total.at[k], second.at[at], second_recv.at[at], first)
    for distance in order:
        if distance % 2 == 0:
            then, (y, x) = place.at(x=1), (0, 1)
        else:
            then, (y, x) = place.at(y=1), (1, 0)
        k = place.at(distance, y, x) // 2
        at = 2 * distance + 1
        arrive(second.at[at], second_recv.at[at])
        total[k] = (wide(total[k]) + wide(second[at])).astype(jnp.bfloat16)
        push(total.at[k], third.at[distance], third_recv.at[distance], then)
    for distance in order:
        k = place.at(distance) // 2
        at = 2 * distance
        arrive(second.at[at], second_recv.at[at])
        arrive(third.at[distance], third_recv.at[distance])
        value = wide(total[k]) + wide(second[at]) + wide(third[distance])
        if distance > 0:
            total[k] = value.astype(jnp.bfloat16)
            push(total.at[k], fourth.at[distance], fourth_recv.at[distance], place.at(distance))
    for distance in range(1, layers):
        arrive(fourth.at[distance], fourth_recv.at[distance])
        value = value + wide(fourth[distance])
    return value, started


def dot_t(left, right):
    return lax.dot_general(
        left, right, (((1,), (1,)), ((), ())), preferred_element_type=jnp.float32
    )


def project_kernel(
    devices,
    x_ref,
    gain_ref,
    routes_ref,
    logits_ref,
    q_ref,
    k_ref,
    v_ref,
    z_ref,
    decay_ref,
    beta_ref,
    columns_ref,
    shares_ref,
    decay_out,
    beta_out,
    buf,
    weights,
    send_sems,
    recv_sems,
    load_sems,
):
    place = Place(devices)
    ready = greet(place)
    width = x_ref.shape[1]
    own = q_ref.shape[0]
    loads = [
        pltpu.make_async_copy(ref, weights.at[pl.ds(i * own, own)], load_sems.at[i])
        for i, ref in enumerate((q_ref, k_ref, v_ref, z_ref))
    ]
    for load in loads:
        load.start()
    normed = (rms_scale(x_ref[...].astype(jnp.float32)) * gain_ref[...]).astype(jnp.bfloat16)
    raised = jnp.exp(logits_ref[...])
    shares = raised / jnp.sum(raised, axis=-1, keepdims=True)
    routes = routes_ref[...]
    lane = lax.broadcasted_iota(jnp.int32, (x_ref.shape[0], LANES), 1)
    share = jnp.zeros(lane.shape, jnp.float32)
    for j in range(routes.shape[1]):
        share = share + jnp.where(lane == routes[:, j : j + 1], shares[:, j : j + 1], 0.0)
    high = share.astype(jnp.bfloat16)
    low = (share - high.astype(jnp.float32)).astype(jnp.bfloat16)
    buf[place.me, :, 0:width] = normed
    buf[place.me, :, width : width + LANES] = high
    buf[place.me, :, width + LANES : width + TAIL] = low
    decay_out[...] = dot_t(normed, decay_ref[...])
    beta_out[...] = dot_t(normed, beta_ref[...])
    ready()
    started = gather_blocks(place, buf, send_sems, recv_sems)
    for load in loads:
        load.wait()
    count = x_ref.shape[0]
    rows = buf[:, :, 0:width].reshape(devices * count, width)
    columns = dot_t(rows, weights[...])
    columns_ref[...] = columns.astype(jnp.bfloat16).reshape(columns_ref.shape)
    shares_ref[...] = buf[:, :, width:]
    settle(started)


def project(devices, x, gain, routes, logits, w_query, w_key, w_value, w_outgate, w_decay, w_beta):
    count, width = x.shape
    own = w_query.shape[1]
    vmem = pl.BlockSpec(memory_space=pltpu.VMEM)
    hbm = pl.BlockSpec(memory_space=pl.ANY)
    heads = w_decay.shape[1]
    return pl.pallas_call(
        functools.partial(project_kernel, devices),
        out_shape=(
            jax.ShapeDtypeStruct((devices, count, 4 * own), jnp.bfloat16),
            jax.ShapeDtypeStruct((devices, count, TAIL), jnp.bfloat16),
            jax.ShapeDtypeStruct((count, heads), jnp.float32),
            jax.ShapeDtypeStruct((count, heads), jnp.float32),
        ),
        in_specs=[vmem] * 4 + [hbm] * 4 + [vmem] * 2,
        out_specs=(vmem,) * 4,
        scratch_shapes=[
            pltpu.VMEM((devices, count, width + TAIL), jnp.bfloat16),
            pltpu.VMEM((4 * own, width), jnp.bfloat16),
            pltpu.SemaphoreType.DMA((gather_sends(devices),)),
            pltpu.SemaphoreType.DMA((devices,)),
            pltpu.SemaphoreType.DMA((4,)),
        ],
        compiler_params=pltpu.CompilerParams(
            collective_id=0, has_side_effects=True, vmem_limit_bytes=32 << 20
        ),
    )(
        x,
        gain[None],
        routes,
        logits,
        w_query.T,
        w_key.T,
        w_value.T,
        w_outgate.T,
        w_decay.T,
        w_beta.T,
    )


def expert_kernel(
    devices,
    branch_ref,
    x_ref,
    gain_mix_ref,
    gain_pre_ref,
    gain_post_ref,
    shares_ref,
    gate_hbm,
    up_hbm,
    down_hbm,
    result_ref,
    buf,
    gate,
    up,
    down,
    hidden,
    weight,
    theirs,
    mine,
    paired,
    total,
    second,
    third,
    fourth,
    gather_send,
    gather_recv,
    load_sems,
    pair_send,
    pair_recv,
    sum_send,
    second_recv,
    third_recv,
    fourth_recv,
):
    place = Place(devices)
    ready = greet(place)
    loads = [
        pltpu.make_async_copy(source, target, load_sems.at[i])
        for i, (source, target) in enumerate(((gate_hbm, gate), (up_hbm, up), (down_hbm, down)))
    ]
    for load in loads:
        load.start()
    count, width = x_ref.shape
    pieces = gate.shape[1]
    pairs = devices // 2
    x_second = x_ref[...].astype(jnp.float32) + rms_scale(branch_ref[...]) * gain_mix_ref[...]
    buf[place.me] = (rms_scale(x_second) * gain_pre_ref[...]).astype(jnp.bfloat16)
    ready()
    started = gather_blocks(place, buf, gather_send, gather_recv)
    share = shares_ref[:, :, 0:LANES].astype(jnp.float32) + shares_ref[:, :, LANES:].astype(
        jnp.float32
    )
    share = share.reshape(devices * count, LANES)
    lane = lax.broadcasted_iota(jnp.int32, share.shape, 1)
    share = jnp.sum(jnp.where(lane == place.me // PIECES, share, 0.0), axis=1, keepdims=True)
    weight[...] = jnp.broadcast_to(share, (devices * count, LANES)).reshape(weight.shape)
    loads[0].wait()
    loads[1].wait()
    rows = buf[...].reshape(devices * count, width)
    step = 256
    for j in range(0, pieces, step):
        gated = clamped_unit(
            jnp.dot(rows, gate[:, j : j + step], preferred_element_type=jnp.float32),
            jnp.dot(rows, up[:, j : j + step], preferred_element_type=jnp.float32),
        )
        hidden[:, :, :, j : j + step] = gated.astype(jnp.bfloat16).reshape(
            pairs, 2, count, step
        )
    loads[2].wait()

    def parts(core, out):
        units = hidden[:, core].reshape(pairs * count, pieces)
        scale = weight[:, core].reshape(pairs * count, LANES)[:, 0:1]
        for j in range(0, width, 512):
            part = jnp.dot(units, down[:, j : j + 512], preferred_element_type=jnp.float32)
            out[:, :, j : j + 512] = (
                (part * scale).astype(jnp.bfloat16).reshape(pairs, count, 512)
            )

    parts(1 - place.core, theirs)
    sent = []
    for distance in range(place.layers - 1, -1, -1):
        for y, x in ((1, 1), (0, 1), (1, 0), (0, 0)):
            k = place.at(distance, y, x) // 2
            copy = remote(
                theirs.at[k],
                paired.at[k],
                pair_send.at[len(sent)],
                pair_recv.at[k],
                place.at(core=1),
            )
            copy.start()
            sent.append(copy)
    parts(place.core, mine)
    moe, more = reduce_blocks(
        place,
        mine,
        paired,
        total,
        second,
        third,
        fourth,
        (pair_recv, sum_send, second_recv, third_recv, fourth_recv),
    )
    result_ref[...] = (x_second + rms_scale(moe) * gain_post_ref[...]).astype(jnp.bfloat16)
    settle(started + sent + more)


def experts_part(
    devices, branch, x, gain_mix, gain_pre, gain_post, shares, w_gate, w_up, w_down
):
    count, width = x.shape
    layers = devices // 8
    pairs = devices // 2
    pieces = w_gate.shape[1]
    vmem = pl.BlockSpec(memory_space=pltpu.VMEM)
    hbm = pl.BlockSpec(memory_space=pl.ANY)
    dma = pltpu.SemaphoreType.DMA

    def blocks(number):
        return pltpu.VMEM((number, count, width), jnp.bfloat16)

    return pl.pallas_call(
        functools.partial(expert_kernel, devices),
        out_shape=jax.ShapeDtypeStruct((count, width), jnp.bfloat16),
        in_specs=[vmem] * 6 + [hbm] * 3,
        out_specs=vmem,
        scratch_shapes=[
            blocks(devices),
            pltpu.VMEM(w_gate.shape, jnp.bfloat16),
            pltpu.VMEM(w_up.shape, jnp.bfloat16),
            pltpu.VMEM(w_down.shape, jnp.bfloat16),
            pltpu.VMEM((pairs, 2, count, pieces), jnp.bfloat16),
            pltpu.VMEM((pairs, 2, count, LANES), jnp.float32),
            blocks(pairs),
            blocks(pairs),
            blocks(pairs),
            blocks(pairs),
            blocks(2 * layers),
            blocks(layers),
            blocks(layers),
            dma((gather_sends(devices),)),
            dma((devices,)),
            dma((3,)),
            dma((pairs,)),
            dma((pairs,)),
            dma((4 * layers,)),
            dma((2 * layers,)),
            dma((layers,)),
            dma((layers,)),
        ],
        compiler_params=pltpu.CompilerParams(
            collective_id=1, has_side_effects=True, vmem_limit_bytes=48 << 20
        ),
    )(
        branch,
        x,
        gain_mix[None],
        gain_pre[None],
        gain_post[None],
        shares,
        w_gate,
        w_up,
        w_down,
    )


def shards(
    residual_in,
    gain_mix_pre,
    w_query,
    w_key,
    w_value,
    w_outgate,
    w_decay,
    w_beta,
    decay_scale,
    decay_bias,
    head_gain,
    w_out,
    gain_mix_post,
    state_cache,
    gain_ffn_pre,
    routes,
    route_logits,
    w_gate,
    w_up,
    w_down,
    gain_ffn_post,
):
    devices = lax.axis_size("ep")
    columns, shares, decay_in, beta_in = project(
        devices,
        residual_in,
        gain_mix_pre,
        routes,
        route_logits,
        w_query,
        w_key,
        w_value,
        w_outgate,
        w_decay,
        w_beta,
    )
    count = residual_in.shape[0]
    joined = lax.all_to_all(columns, "ep", split_axis=0, concat_axis=0, tiled=True)
    joined = joined.reshape(devices, count, 4, -1).transpose(2, 1, 0, 3).reshape(4, count, H * HD)
    mixed, new_state = delta_step(
        joined[0],
        joined[1],
        joined[2],
        joined[3],
        decay_in,
        beta_in,
        state_cache,
        decay_scale,
        decay_bias,
        head_gain,
    )
    branch = jnp.dot(mixed, w_out, preferred_element_type=jnp.float32)
    result = experts_part(
        devices,
        branch,
        residual_in,
        gain_mix_post,
        gain_ffn_pre,
        gain_ffn_post,
        shares,
        w_gate,
        w_up,
        w_down,
    )
    return (result, new_state)


def solution(mesh):
    in_specs = (
        P("ep", None),
        P(),
        P(None, "ep"),
        P(None, "ep"),
        P(None, "ep"),
        P(None, "ep"),
        P(),
        P(),
        P(),
        P(),
        P(),
        P(),
        P(),
        P("ep", None, None, None),
        P(),
        P("ep", None),
        P("ep", None),
        P(None, "ep"),
        P(None, "ep"),
        P("ep", None),
        P(),
    )
    out_specs = (P("ep", None), P("ep", None, None, None))
    return jax.shard_map(shards, mesh=mesh, in_specs=in_specs, out_specs=out_specs, check_vma=False)
```

```python
import functools

import jax
import jax.numpy as jnp
from jax import lax
from jax.experimental import pallas as pl
from jax.experimental.pallas import tpu as pltpu
from jax.sharding import PartitionSpec as P

H = 16
HD = 128
PIECES = 4
TOPK = 4
LANES = 128
TAIL = 2 * LANES
MESH = pl.DeviceIdType.MESH

EPS = 1e-06
LIMIT = 7.0
ALPHA = 1.702


def rms_scale(values):
    return values * lax.rsqrt(jnp.mean(values * values, axis=-1, keepdims=True) + EPS)


def clamped_unit(gate, upper):
    glu = jnp.minimum(gate, LIMIT)
    linear = jnp.clip(upper, -LIMIT, LIMIT)
    return glu * jax.nn.sigmoid(ALPHA * glu) * (linear + 1.0)


def flipped(value, distance):
    bit = 1
    while bit <= distance:
        if distance & bit:
            value = value + bit - 2 * bit * (lax.rem(value // bit, 2))
        bit *= 2
    return value


class Place:
    def __init__(self, devices):
        self.devices = devices
        self.layers = devices // 8
        self.me = lax.axis_index("ep")
        self.core = lax.rem(self.me, 2)
        self.x = lax.rem(self.me // 2, 2)
        self.y = lax.rem(self.me // 4, 2)
        self.z = self.me // 8

    def at(self, distance=0, y=0, x=0, core=0):
        z = flipped(self.z, distance)
        return (
            z * 8
            + flipped(self.y, y) * 4
            + flipped(self.x, x) * 2
            + flipped(self.core, core)
        )

    def partners(self):
        return [self.at(d) for d in range(1, self.layers)] + [
            self.at(y=1),
            self.at(x=1),
            self.at(core=1),
        ]


def greet(partners):
    barrier = pltpu.get_barrier_semaphore()
    for partner in partners:
        pl.semaphore_signal(barrier, inc=1, device_id=(partner,), device_id_type=MESH)
    return lambda: pl.semaphore_wait(barrier, len(partners))


def load_all(pairs, sems):
    loads = [
        pltpu.make_async_copy(source, target, sems.at[i])
        for i, (source, target) in enumerate(pairs)
    ]
    for load in loads:
        load.start()
    return loads


def remote(source, target, send_sem, recv_sem, device):
    return pltpu.make_async_remote_copy(
        src_ref=source,
        dst_ref=target,
        send_sem=send_sem,
        recv_sem=recv_sem,
        device_id=(device,),
        device_id_type=MESH,
    )


def gather_sends(devices):
    layers = devices // 8
    return layers - 1 + 3 * layers + devices // 2


def gather_blocks(place, buf, send_sems, recv_sems):
    started = []

    def push(block, device):
        copy = remote(
            buf.at[block], buf.at[block], send_sems.at[len(started)], recv_sems.at[block], device
        )
        copy.start()
        started.append(copy)

    def arrive(block):
        remote(
            buf.at[block], buf.at[block], send_sems.at[0], recv_sems.at[block], place.at(core=1)
        ).wait_recv()

    def spread(distance):
        block = place.at(distance)
        push(block, place.at(x=1))
        push(block, place.at(y=1))
        push(block, place.at(core=1))

    def onward(distance):
        across_x, across_y = place.at(distance, x=1), place.at(distance, y=1)
        arrive(across_x)
        if distance % 2 == 0:
            push(across_x, place.at(y=1))
        push(across_x, place.at(core=1))
        arrive(across_y)
        if distance % 2 == 1:
            push(across_y, place.at(x=1))
        push(across_y, place.at(core=1))

    layers = place.layers
    for distance in range(layers - 1, 0, -1):
        push(place.me, place.at(distance))
    spread(0)
    for distance in range(1, layers):
        arrive(place.at(distance))
        spread(distance)
        onward(distance - 1)
    onward(layers - 1)
    for distance in range(layers):
        diagonal = place.at(distance, y=1, x=1)
        arrive(diagonal)
        push(diagonal, place.at(core=1))
    for distance in range(layers):
        for y in range(2):
            for x in range(2):
                arrive(place.at(distance, y, x, 1))
    return started


def settle(started):
    for copy in started:
        copy.wait_send()


def reduce_blocks(place, mine, paired, total, second, third, fourth, sems):
    pair_recv, send_sems, second_recv, third_recv, fourth_recv = sems
    started = []
    layers = place.layers

    def push(source, target, recv_sem, device):
        copy = remote(source, target, send_sems.at[len(started)], recv_sem, device)
        copy.start()
        started.append(copy)

    def arrive(target, recv_sem):
        remote(target, target, send_sems.at[0], recv_sem, place.at(core=1)).wait_recv()

    def wide(block):
        return block.astype(jnp.float32)

    order = list(range(layers - 1, -1, -1))
    for distance in order:
        for y, x in ((1, 1), (0, 1), (1, 0), (0, 0)):
            k = place.at(distance, y, x) // 2
            arrive(paired.at[k], pair_recv.at[k])
            total[k] = (wide(mine[k]) + wide(paired[k])).astype(jnp.bfloat16)
    for distance in order:
        if distance % 2 == 0:
            first, far, near = place.at(y=1), (1, 1), (1, 0)
        else:
            first, far, near = place.at(x=1), (1, 1), (0, 1)
        for slot, (y, x) in ((1, far), (0, near)):
            k = place.at(distance, y, x) // 2
            at = 2 * distance + slot
            push(total.at[k], second.at[at], second_recv.at[at], first)
    for distance in order:
        if distance % 2 == 0:
            then, (y, x) = place.at(x=1), (0, 1)
        else:
            then, (y, x) = place.at(y=1), (1, 0)
        k = place.at(distance, y, x) // 2
        at = 2 * distance + 1
        arrive(second.at[at], second_recv.at[at])
        total[k] = (wide(total[k]) + wide(second[at])).astype(jnp.bfloat16)
        push(total.at[k], third.at[distance], third_recv.at[distance], then)
    for distance in order:
        k = place.at(distance) // 2
        at = 2 * distance
        arrive(second.at[at], second_recv.at[at])
        arrive(third.at[distance], third_recv.at[distance])
        value = wide(total[k]) + wide(second[at]) + wide(third[distance])
        if distance > 0:
            total[k] = value.astype(jnp.bfloat16)
            push(total.at[k], fourth.at[distance], fourth_recv.at[distance], place.at(distance))
    for distance in range(1, layers):
        arrive(fourth.at[distance], fourth_recv.at[distance])
        value = value + wide(fourth[distance])
    return value, started


def dot_t(left, right):
    return lax.dot_general(
        left, right, (((1,), (1,)), ((), ())), preferred_element_type=jnp.float32
    )


def column_of(row):
    size = row.shape[1]
    across = lax.broadcasted_iota(jnp.int32, (size, size), 1)
    down = lax.broadcasted_iota(jnp.int32, (size, size), 0)
    return jnp.sum(
        jnp.where(across == down, jnp.broadcast_to(row, (size, size)), 0.0), axis=1, keepdims=True
    )


def project_kernel(
    devices,
    own,
    x_hbm,
    gain_hbm,
    routes_hbm,
    logits_hbm,
    decay_hbm,
    beta_hbm,
    q_hbm,
    k_hbm,
    v_hbm,
    z_hbm,
    joined,
    shares_ref,
    decay_out,
    beta_out,
    x_ref,
    gain_ref,
    routes_ref,
    logits_ref,
    decay_ref,
    beta_ref,
    weights,
    buf,
    columns,
    send_sems,
    recv_sems,
    out_sems,
    in_sems,
    load_sems,
):
    place = Place(devices)
    others = [lax.rem(place.me + i, devices) for i in range(1, devices)]
    ready = greet(others)
    count, width = x_ref.shape
    loads = load_all(
        [
            (x_hbm, x_ref),
            (gain_hbm, gain_ref),
            (routes_hbm, routes_ref),
            (logits_hbm, logits_ref),
            (decay_hbm, decay_ref),
            (beta_hbm, beta_ref),
        ]
        + [
            (ref, weights.at[pl.ds(i * own, own)])
            for i, ref in enumerate((q_hbm, k_hbm, v_hbm, z_hbm))
        ],
        load_sems,
    )
    for load in loads[:4]:
        load.wait()
    normed = (rms_scale(x_ref[...].astype(jnp.float32)) * gain_ref[...]).astype(jnp.bfloat16)
    raised = jnp.exp(logits_ref[...])
    shares = raised / jnp.sum(raised, axis=0, keepdims=True)
    routes = routes_ref[...].astype(jnp.float32)
    lane = lax.broadcasted_iota(jnp.int32, (count, LANES), 1).astype(jnp.float32)
    share = jnp.zeros(lane.shape, jnp.float32)
    for j in range(routes.shape[0]):
        share = share + jnp.where(
            lane == column_of(routes[j : j + 1]), column_of(shares[j : j + 1]), 0.0
        )
    high = share.astype(jnp.bfloat16)
    low = (share - high.astype(jnp.float32)).astype(jnp.bfloat16)
    buf[place.me, :, 0:width] = normed
    buf[place.me, :, width : width + LANES] = high
    buf[place.me, :, width + LANES : width + TAIL] = low
    ready()
    started = gather_blocks(place, buf, send_sems, recv_sems)
    for load in loads[4:]:
        load.wait()
    rows = buf[:, :, 0:width].reshape(devices * count, width)
    columns[...] = dot_t(rows, weights[...]).astype(jnp.bfloat16).reshape(columns.shape)
    for i, other in enumerate(others):
        copy = remote(
            columns.at[other], joined.at[place.me], out_sems.at[i], in_sems.at[place.me], other
        )
        copy.start()
        started.append(copy)
    joined[place.me] = columns[place.me]
    decay_out[...] = dot_t(normed, decay_ref[...])
    beta_out[...] = dot_t(normed, beta_ref[...])
    shares_ref[...] = buf[:, :, width:]
    for other in others:
        remote(
            columns.at[other], joined.at[other], out_sems.at[0], in_sems.at[other], other
        ).wait_recv()
    settle(started)


def project(devices, x, gain, routes, logits, w_query, w_key, w_value, w_outgate, w_decay, w_beta):
    count, width = x.shape
    own = w_query.shape[1]
    block = max(4 * own, LANES)
    vmem = pl.BlockSpec(memory_space=pltpu.VMEM)
    hbm = pl.BlockSpec(memory_space=pltpu.HBM)
    heads = w_decay.shape[1]
    dma = pltpu.SemaphoreType.DMA
    inputs = (
        x,
        gain[None],
        routes.T,
        logits.T,
        w_decay.T,
        w_beta.T,
        w_query.T,
        w_key.T,
        w_value.T,
        w_outgate.T,
    )
    return pl.pallas_call(
        functools.partial(project_kernel, devices, own),
        out_shape=(
            jax.ShapeDtypeStruct((devices, count, block), jnp.bfloat16),
            jax.ShapeDtypeStruct((devices, count, TAIL), jnp.bfloat16),
            jax.ShapeDtypeStruct((count, heads), jnp.float32),
            jax.ShapeDtypeStruct((count, heads), jnp.float32),
        ),
        in_specs=[hbm] * len(inputs),
        out_specs=(vmem,) * 4,
        scratch_shapes=[pltpu.VMEM(a.shape, a.dtype) for a in inputs[:6]]
        + [
            pltpu.VMEM((block, width), jnp.bfloat16),
            pltpu.VMEM((devices, count, width + TAIL), jnp.bfloat16),
            pltpu.VMEM((devices, count, block), jnp.bfloat16),
            dma((gather_sends(devices),)),
            dma((devices,)),
            dma((devices,)),
            dma((devices,)),
            dma((len(inputs),)),
        ],
        compiler_params=pltpu.CompilerParams(
            collective_id=0, has_side_effects=True, vmem_limit_bytes=20 << 20
        ),
    )(*inputs)


def head_rows(joined, head, kind, own):
    lane = lax.broadcasted_iota(jnp.int32, (joined.shape[1], LANES), 1)
    value = jnp.zeros(lane.shape, jnp.float32)
    group, offset = divmod(kind * own, LANES)
    for i in range(HD // own):
        piece = joined[head * (HD // own) + i, :, group * LANES : (group + 1) * LANES]
        piece = piece.astype(jnp.float32)
        shift = (i * own - offset) % LANES
        if shift:
            piece = pltpu.roll(piece, shift, 1)
        value = jnp.where((lane >= i * own) & (lane < (i + 1) * own), piece, value)
    return value


def delta_kernel(
    own,
    joined,
    decay_in,
    beta_in,
    scale_ref,
    bias_ref,
    head_gain_ref,
    state_hbm,
    w_out_hbm,
    branch_ref,
    new_hbm,
    state,
    fresh,
    w_out,
    mixed,
    state_sems,
    fresh_sems,
    out_sems,
):
    heads = mixed.shape[0]
    count = state.shape[0]
    width = w_out.shape[1]

    def state_in(h):
        return pltpu.make_async_copy(state_hbm.at[:, h], state.at[:, h], state_sems.at[h])

    def state_out(h):
        return pltpu.make_async_copy(fresh.at[:, h], new_hbm.at[:, h], fresh_sems.at[h])

    for h in range(heads):
        state_in(h).start()
    w_load = pltpu.make_async_copy(w_out_hbm, w_out, out_sems.at[0])
    w_load.start()
    decay = jnp.exp(-scale_ref[...] * jax.nn.softplus(decay_in[...] + bias_ref[...]))
    strength = jax.nn.sigmoid(beta_in[...])
    lane = lax.broadcasted_iota(jnp.int32, decay.shape, 1)

    def one(h, carry):
        query = jax.nn.silu(head_rows(joined, h, 0, own))
        query = (
            query * lax.rsqrt(jnp.sum(query * query, axis=-1, keepdims=True) + EPS) * HD ** (-0.5)
        )
        keys = jax.nn.silu(head_rows(joined, h, 1, own))
        keys = keys * lax.rsqrt(jnp.sum(keys * keys, axis=-1, keepdims=True) + EPS)
        values = jax.nn.silu(head_rows(joined, h, 2, own))
        outgate = jax.nn.silu(head_rows(joined, h, 3, own))
        keep = jnp.sum(jnp.where(lane == h, decay, 0.0), axis=1, keepdims=True)
        beta = jnp.sum(jnp.where(lane == h, strength, 0.0), axis=1, keepdims=True)
        overlap = jnp.sum(keys * query, axis=1, keepdims=True)
        upright = jnp.transpose(jnp.concatenate([keys, query], axis=0))
        state_in(h).wait()
        outputs = []
        for r in range(count):
            held = state[r, h].astype(jnp.float32)
            key = jnp.broadcast_to(upright[:, r : r + 1], held.shape)
            ask = jnp.broadcast_to(upright[:, count + r : count + r + 1], held.shape)
            rate = keep[r : r + 1]
            guess = rate * jnp.sum(key * held, axis=0, keepdims=True)
            change = beta[r : r + 1] * (values[r : r + 1] - guess)
            seen = rate * jnp.sum(ask * held, axis=0, keepdims=True)
            outputs.append(seen + overlap[r : r + 1] * change)
            fresh[r, h] = (rate * held + key * change).astype(jnp.bfloat16)
        state_out(h).start()
        output = rms_scale(jnp.concatenate(outputs, axis=0)) * head_gain_ref[...]
        mixed[h] = (output * outgate).astype(jnp.bfloat16)
        return carry

    lax.fori_loop(0, heads, one, 0)
    w_load.wait()
    rows = jnp.concatenate([mixed[h] for h in range(heads)], axis=1)
    for j in range(0, width, 512):
        branch_ref[:, j : j + 512] = jnp.dot(
            rows, w_out[:, j : j + 512], preferred_element_type=jnp.float32
        )
    for h in range(heads):
        state_out(h).wait()


def delta_part(own, joined, decay_in, beta_in, scale, bias, head_gain, state, w_out):
    count, heads = state.shape[:2]
    vmem = pl.BlockSpec(memory_space=pltpu.VMEM)
    hbm = pl.BlockSpec(memory_space=pltpu.HBM)
    dma = pltpu.SemaphoreType.DMA
    return pl.pallas_call(
        functools.partial(delta_kernel, own),
        out_shape=(
            jax.ShapeDtypeStruct((count, w_out.shape[1]), jnp.float32),
            jax.ShapeDtypeStruct(state.shape, state.dtype),
        ),
        in_specs=[vmem] * 6 + [hbm] * 2,
        out_specs=(vmem, hbm),
        scratch_shapes=[
            pltpu.VMEM(state.shape, state.dtype),
            pltpu.VMEM(state.shape, state.dtype),
            pltpu.VMEM(w_out.shape, w_out.dtype),
            pltpu.VMEM((heads, count, HD), jnp.bfloat16),
            dma((heads,)),
            dma((heads,)),
            dma((1,)),
        ],
        compiler_params=pltpu.CompilerParams(vmem_limit_bytes=40 << 20),
    )(joined, decay_in, beta_in, scale[None], bias[None], head_gain[None], state, w_out)


def expert_kernel(
    devices,
    branch_ref,
    shares_ref,
    x_hbm,
    gain_mix_hbm,
    gain_pre_hbm,
    gain_post_hbm,
    gate_hbm,
    up_hbm,
    down_hbm,
    result_ref,
    x_ref,
    gain_mix_ref,
    gain_pre_ref,
    gain_post_ref,
    small_sems,
    buf,
    gate,
    up,
    down,
    hidden,
    weight,
    theirs,
    mine,
    paired,
    total,
    second,
    third,
    fourth,
    gather_send,
    gather_recv,
    load_sems,
    pair_send,
    pair_recv,
    sum_send,
    second_recv,
    third_recv,
    fourth_recv,
):
    place = Place(devices)
    ready = greet(place.partners())
    small = load_all(
        [
            (x_hbm, x_ref),
            (gain_mix_hbm, gain_mix_ref),
            (gain_pre_hbm, gain_pre_ref),
            (gain_post_hbm, gain_post_ref),
        ],
        small_sems,
    )
    loads = load_all([(gate_hbm, gate), (up_hbm, up), (down_hbm, down)], load_sems)
    for load in small:
        load.wait()
    count, width = x_ref.shape
    pieces = gate.shape[1]
    pairs = devices // 2
    x_second = x_ref[...].astype(jnp.float32) + rms_scale(branch_ref[...]) * gain_mix_ref[...]
    buf[place.me] = (rms_scale(x_second) * gain_pre_ref[...]).astype(jnp.bfloat16)
    ready()
    started = gather_blocks(place, buf, gather_send, gather_recv)
    share = shares_ref[:, :, 0:LANES].astype(jnp.float32) + shares_ref[:, :, LANES:].astype(
        jnp.float32
    )
    share = share.reshape(devices * count, LANES)
    lane = lax.broadcasted_iota(jnp.int32, share.shape, 1)
    share = jnp.sum(jnp.where(lane == place.me // PIECES, share, 0.0), axis=1, keepdims=True)
    weight[...] = jnp.broadcast_to(share, (devices * count, LANES)).reshape(weight.shape)
    loads[0].wait()
    loads[1].wait()
    rows = buf[...].reshape(devices * count, width)
    step = 256
    for j in range(0, pieces, step):
        gated = clamped_unit(
            jnp.dot(rows, gate[:, j : j + step], preferred_element_type=jnp.float32),
            jnp.dot(rows, up[:, j : j + step], preferred_element_type=jnp.float32),
        )
        hidden[:, :, :, j : j + step] = gated.astype(jnp.bfloat16).reshape(
            pairs, 2, count, step
        )
    loads[2].wait()

    def parts(core, out):
        units = hidden[:, core].reshape(pairs * count, pieces)
        scale = weight[:, core].reshape(pairs * count, LANES)[:, 0:1]
        for j in range(0, width, 512):
            part = jnp.dot(units, down[:, j : j + 512], preferred_element_type=jnp.float32)
            out[:, :, j : j + 512] = (
                (part * scale).astype(jnp.bfloat16).reshape(pairs, count, 512)
            )

    parts(1 - place.core, theirs)
    sent = []
    for distance in range(place.layers - 1, -1, -1):
        for y, x in ((1, 1), (0, 1), (1, 0), (0, 0)):
            k = place.at(distance, y, x) // 2
            copy = remote(
                theirs.at[k],
                paired.at[k],
                pair_send.at[len(sent)],
                pair_recv.at[k],
                place.at(core=1),
            )
            copy.start()
            sent.append(copy)
    parts(place.core, mine)
    moe, more = reduce_blocks(
        place,
        mine,
        paired,
        total,
        second,
        third,
        fourth,
        (pair_recv, sum_send, second_recv, third_recv, fourth_recv),
    )
    result_ref[...] = (x_second + rms_scale(moe) * gain_post_ref[...]).astype(jnp.bfloat16)
    settle(started + sent + more)


def experts_part(
    devices, branch, x, gain_mix, gain_pre, gain_post, shares, w_gate, w_up, w_down
):
    count, width = x.shape
    layers = devices // 8
    pairs = devices // 2
    pieces = w_gate.shape[1]
    vmem = pl.BlockSpec(memory_space=pltpu.VMEM)
    hbm = pl.BlockSpec(memory_space=pltpu.HBM)
    dma = pltpu.SemaphoreType.DMA

    def blocks(number):
        return pltpu.VMEM((number, count, width), jnp.bfloat16)

    return pl.pallas_call(
        functools.partial(expert_kernel, devices),
        out_shape=jax.ShapeDtypeStruct((count, width), jnp.bfloat16),
        in_specs=[vmem] * 2 + [hbm] * 7,
        out_specs=vmem,
        scratch_shapes=[
            pltpu.VMEM(x.shape, x.dtype),
            pltpu.VMEM((1, width), jnp.float32),
            pltpu.VMEM((1, width), jnp.float32),
            pltpu.VMEM((1, width), jnp.float32),
            dma((4,)),
            blocks(devices),
            pltpu.VMEM(w_gate.shape, jnp.bfloat16),
            pltpu.VMEM(w_up.shape, jnp.bfloat16),
            pltpu.VMEM(w_down.shape, jnp.bfloat16),
            pltpu.VMEM((pairs, 2, count, pieces), jnp.bfloat16),
            pltpu.VMEM((pairs, 2, count, LANES), jnp.float32),
            blocks(pairs),
            blocks(pairs),
            blocks(pairs),
            blocks(pairs),
            blocks(2 * layers),
            blocks(layers),
            blocks(layers),
            dma((gather_sends(devices),)),
            dma((devices,)),
            dma((3,)),
            dma((pairs,)),
            dma((pairs,)),
            dma((4 * layers,)),
            dma((2 * layers,)),
            dma((layers,)),
            dma((layers,)),
        ],
        compiler_params=pltpu.CompilerParams(
            collective_id=1, has_side_effects=True, vmem_limit_bytes=48 << 20
        ),
    )(
        branch,
        shares,
        x,
        gain_mix[None],
        gain_pre[None],
        gain_post[None],
        w_gate,
        w_up,
        w_down,
    )


def shards(
    residual_in,
    gain_mix_pre,
    w_query,
    w_key,
    w_value,
    w_outgate,
    w_decay,
    w_beta,
    decay_scale,
    decay_bias,
    head_gain,
    w_out,
    gain_mix_post,
    state_cache,
    gain_ffn_pre,
    routes,
    route_logits,
    w_gate,
    w_up,
    w_down,
    gain_ffn_post,
):
    devices = lax.axis_size("ep")
    joined, shares, decay_in, beta_in = project(
        devices,
        residual_in,
        gain_mix_pre,
        routes,
        route_logits,
        w_query,
        w_key,
        w_value,
        w_outgate,
        w_decay,
        w_beta,
    )
    branch, new_state = delta_part(
        w_query.shape[1],
        joined,
        decay_in,
        beta_in,
        decay_scale,
        decay_bias,
        head_gain,
        state_cache,
        w_out,
    )
    result = experts_part(
        devices,
        branch,
        residual_in,
        gain_mix_post,
        gain_ffn_pre,
        gain_ffn_post,
        shares,
        w_gate,
        w_up,
        w_down,
    )
    return (result, new_state)


def solution(mesh):
    in_specs = (
        P("ep", None),
        P(),
        P(None, "ep"),
        P(None, "ep"),
        P(None, "ep"),
        P(None, "ep"),
        P(),
        P(),
        P(),
        P(),
        P(),
        P(),
        P(),
        P("ep", None, None, None),
        P(),
        P("ep", None),
        P("ep", None),
        P(None, "ep"),
        P(None, "ep"),
        P("ep", None),
        P(),
    )
    out_specs = (P("ep", None), P("ep", None, None, None))
    return jax.shard_map(shards, mesh=mesh, in_specs=in_specs, out_specs=out_specs, check_vma=False)
```

```python
import functools

import jax
import jax.numpy as jnp
from jax import lax
from jax.experimental import pallas as pl
from jax.experimental.pallas import tpu as pltpu
from jax.sharding import PartitionSpec as P

H = 16
HD = 128
PIECES = 4
TOPK = 4
LANES = 128
TAIL = 2 * LANES
VMEM_LIMIT = 66 * 1000 * 1000
MESH = pl.DeviceIdType.MESH

EPS = 1e-06
LIMIT = 7.0
ALPHA = 1.702


def rms_scale(values):
    return values * lax.rsqrt(jnp.mean(values * values, axis=-1, keepdims=True) + EPS)


def clamped_unit(gate, upper):
    glu = jnp.minimum(gate, LIMIT)
    linear = jnp.clip(upper, -LIMIT, LIMIT)
    return glu * jax.nn.sigmoid(ALPHA * glu) * (linear + 1.0)


def flipped(value, distance):
    bit = 1
    while bit <= distance:
        if distance & bit:
            value = value + bit - 2 * bit * (lax.rem(value // bit, 2))
        bit *= 2
    return value


class Place:
    def __init__(self, devices):
        self.devices = devices
        self.layers = devices // 8
        self.me = lax.axis_index("ep")
        self.core = lax.rem(self.me, 2)
        self.x = lax.rem(self.me // 2, 2)
        self.y = lax.rem(self.me // 4, 2)
        self.z = self.me // 8

    def at(self, distance=0, y=0, x=0, core=0):
        z = flipped(self.z, distance)
        return (
            z * 8
            + flipped(self.y, y) * 4
            + flipped(self.x, x) * 2
            + flipped(self.core, core)
        )

    def partners(self):
        return [self.at(d) for d in range(1, self.layers)] + [
            self.at(y=1),
            self.at(x=1),
            self.at(core=1),
        ]


def greet(partners):
    barrier = pltpu.get_barrier_semaphore()
    for partner in partners:
        pl.semaphore_signal(barrier, inc=1, device_id=(partner,), device_id_type=MESH)
    return lambda: pl.semaphore_wait(barrier, len(partners))


def load_all(pairs, sems):
    loads = [
        pltpu.make_async_copy(source, target, sems.at[i])
        for i, (source, target) in enumerate(pairs)
    ]
    for load in loads:
        load.start()
    return loads


def remote(source, target, send_sem, recv_sem, device):
    return pltpu.make_async_remote_copy(
        src_ref=source,
        dst_ref=target,
        send_sem=send_sem,
        recv_sem=recv_sem,
        device_id=(device,),
        device_id_type=MESH,
    )


def gather_sends(devices):
    layers = devices // 8
    return layers - 1 + 3 * layers + devices // 2


def gather_blocks(place, buf, send_sems, recv_sems):
    started = []

    def push(block, device):
        copy = remote(
            buf.at[block], buf.at[block], send_sems.at[len(started)], recv_sems.at[block], device
        )
        copy.start()
        started.append(copy)

    def arrive(block):
        remote(
            buf.at[block], buf.at[block], send_sems.at[0], recv_sems.at[block], place.at(core=1)
        ).wait_recv()

    def spread(distance):
        block = place.at(distance)
        push(block, place.at(x=1))
        push(block, place.at(y=1))
        push(block, place.at(core=1))

    def onward(distance):
        across_x, across_y = place.at(distance, x=1), place.at(distance, y=1)
        arrive(across_x)
        if distance % 2 == 0:
            push(across_x, place.at(y=1))
        push(across_x, place.at(core=1))
        arrive(across_y)
        if distance % 2 == 1:
            push(across_y, place.at(x=1))
        push(across_y, place.at(core=1))

    layers = place.layers
    for distance in range(layers - 1, 0, -1):
        push(place.me, place.at(distance))
    spread(0)
    for distance in range(1, layers):
        arrive(place.at(distance))
        spread(distance)
        onward(distance - 1)
    onward(layers - 1)
    for distance in range(layers):
        diagonal = place.at(distance, y=1, x=1)
        arrive(diagonal)
        push(diagonal, place.at(core=1))
    for distance in range(layers):
        for y in range(2):
            for x in range(2):
                arrive(place.at(distance, y, x, 1))
    return started


def settle(started):
    for copy in started:
        copy.wait_send()


def reduce_blocks(place, mine, paired, total, second, third, fourth, sems):
    pair_recv, send_sems, second_recv, third_recv, fourth_recv = sems
    started = []
    layers = place.layers

    def push(source, target, recv_sem, device):
        copy = remote(source, target, send_sems.at[len(started)], recv_sem, device)
        copy.start()
        started.append(copy)

    def arrive(target, recv_sem):
        remote(target, target, send_sems.at[0], recv_sem, place.at(core=1)).wait_recv()

    def wide(block):
        return block.astype(jnp.float32)

    order = list(range(layers - 1, -1, -1))
    for distance in order:
        for y, x in ((1, 1), (0, 1), (1, 0), (0, 0)):
            k = place.at(distance, y, x) // 2
            arrive(paired.at[k], pair_recv.at[k])
            total[k] = (wide(mine[k]) + wide(paired[k])).astype(jnp.bfloat16)
    for distance in order:
        if distance % 2 == 0:
            first, far, near = place.at(y=1), (1, 1), (1, 0)
        else:
            first, far, near = place.at(x=1), (1, 1), (0, 1)
        for slot, (y, x) in ((1, far), (0, near)):
            k = place.at(distance, y, x) // 2
            at = 2 * distance + slot
            push(total.at[k], second.at[at], second_recv.at[at], first)
    for distance in order:
        if distance % 2 == 0:
            then, (y, x) = place.at(x=1), (0, 1)
        else:
            then, (y, x) = place.at(y=1), (1, 0)
        k = place.at(distance, y, x) // 2
        at = 2 * distance + 1
        arrive(second.at[at], second_recv.at[at])
        total[k] = (wide(total[k]) + wide(second[at])).astype(jnp.bfloat16)
        push(total.at[k], third.at[distance], third_recv.at[distance], then)
    for distance in order:
        k = place.at(distance) // 2
        at = 2 * distance
        arrive(second.at[at], second_recv.at[at])
        arrive(third.at[distance], third_recv.at[distance])
        value = wide(total[k]) + wide(second[at]) + wide(third[distance])
        if distance > 0:
            total[k] = value.astype(jnp.bfloat16)
            push(total.at[k], fourth.at[distance], fourth_recv.at[distance], place.at(distance))
    for distance in range(1, layers):
        arrive(fourth.at[distance], fourth_recv.at[distance])
        value = value + wide(fourth[distance])
    return value, started


def dot_t(left, right):
    return lax.dot_general(
        left, right, (((1,), (1,)), ((), ())), preferred_element_type=jnp.float32
    )


def column_of(row):
    size = row.shape[1]
    across = lax.broadcasted_iota(jnp.int32, (size, size), 1)
    down = lax.broadcasted_iota(jnp.int32, (size, size), 0)
    return jnp.sum(
        jnp.where(across == down, jnp.broadcast_to(row, (size, size)), 0.0), axis=1, keepdims=True
    )


def project_kernel(
    devices,
    own,
    x_hbm,
    gain_hbm,
    routes_hbm,
    logits_hbm,
    decay_hbm,
    beta_hbm,
    q_hbm,
    k_hbm,
    v_hbm,
    z_hbm,
    joined,
    shares_ref,
    decay_out,
    beta_out,
    x_ref,
    gain_ref,
    routes_ref,
    logits_ref,
    decay_ref,
    beta_ref,
    weights,
    buf,
    columns,
    send_sems,
    recv_sems,
    out_sems,
    in_sems,
    load_sems,
):
    place = Place(devices)
    others = [lax.rem(place.me + i, devices) for i in range(1, devices)]
    ready = greet(others)
    count, width = x_ref.shape
    loads = load_all(
        [
            (x_hbm, x_ref),
            (gain_hbm, gain_ref),
            (routes_hbm, routes_ref),
            (logits_hbm, logits_ref),
            (decay_hbm, decay_ref),
            (beta_hbm, beta_ref),
        ]
        + [
            (ref, weights.at[pl.ds(i * own, own)])
            for i, ref in enumerate((q_hbm, k_hbm, v_hbm, z_hbm))
        ],
        load_sems,
    )
    for load in loads[:4]:
        load.wait()
    normed = (rms_scale(x_ref[...].astype(jnp.float32)) * gain_ref[...]).astype(jnp.bfloat16)
    raised = jnp.exp(logits_ref[...])
    shares = raised / jnp.sum(raised, axis=0, keepdims=True)
    routes = routes_ref[...].astype(jnp.float32)
    lane = lax.broadcasted_iota(jnp.int32, (count, LANES), 1).astype(jnp.float32)
    share = jnp.zeros(lane.shape, jnp.float32)
    for j in range(routes.shape[0]):
        share = share + jnp.where(
            lane == column_of(routes[j : j + 1]), column_of(shares[j : j + 1]), 0.0
        )
    high = share.astype(jnp.bfloat16)
    low = (share - high.astype(jnp.float32)).astype(jnp.bfloat16)
    buf[place.me, :, 0:width] = normed
    buf[place.me, :, width : width + LANES] = high
    buf[place.me, :, width + LANES : width + TAIL] = low
    ready()
    started = gather_blocks(place, buf, send_sems, recv_sems)
    for load in loads[4:]:
        load.wait()
    rows = buf[:, :, 0:width].reshape(devices * count, width)
    columns[...] = dot_t(rows, weights[...]).astype(jnp.bfloat16).reshape(columns.shape)
    for i, other in enumerate(others):
        copy = remote(
            columns.at[other], joined.at[place.me], out_sems.at[i], in_sems.at[place.me], other
        )
        copy.start()
        started.append(copy)
    joined[place.me] = columns[place.me]
    decay_out[...] = dot_t(normed, decay_ref[...])
    beta_out[...] = dot_t(normed, beta_ref[...])
    shares_ref[...] = buf[:, :, width:]
    for other in others:
        remote(
            columns.at[other], joined.at[other], out_sems.at[0], in_sems.at[other], other
        ).wait_recv()
    settle(started)


def project(devices, x, gain, routes, logits, w_query, w_key, w_value, w_outgate, w_decay, w_beta):
    count, width = x.shape
    own = w_query.shape[1]
    block = max(4 * own, LANES)
    vmem = pl.BlockSpec(memory_space=pltpu.VMEM)
    hbm = pl.BlockSpec(memory_space=pltpu.HBM)
    heads = w_decay.shape[1]
    dma = pltpu.SemaphoreType.DMA
    inputs = (
        x,
        gain[None],
        routes.T,
        logits.T,
        w_decay.T,
        w_beta.T,
        w_query.T,
        w_key.T,
        w_value.T,
        w_outgate.T,
    )
    return pl.pallas_call(
        functools.partial(project_kernel, devices, own),
        out_shape=(
            jax.ShapeDtypeStruct((devices, count, block), jnp.bfloat16),
            jax.ShapeDtypeStruct((devices, count, TAIL), jnp.bfloat16),
            jax.ShapeDtypeStruct((count, heads), jnp.float32),
            jax.ShapeDtypeStruct((count, heads), jnp.float32),
        ),
        in_specs=[hbm] * len(inputs),
        out_specs=(vmem,) * 4,
        scratch_shapes=[pltpu.VMEM(a.shape, a.dtype) for a in inputs[:6]]
        + [
            pltpu.VMEM((block, width), jnp.bfloat16),
            pltpu.VMEM((devices, count, width + TAIL), jnp.bfloat16),
            pltpu.VMEM((devices, count, block), jnp.bfloat16),
            dma((gather_sends(devices),)),
            dma((devices,)),
            dma((devices,)),
            dma((devices,)),
            dma((len(inputs),)),
        ],
        compiler_params=pltpu.CompilerParams(
            collective_id=0, has_side_effects=True, vmem_limit_bytes=VMEM_LIMIT
        ),
    )(*inputs)


def head_rows(joined, head, kind, own):
    lane = lax.broadcasted_iota(jnp.int32, (joined.shape[1], LANES), 1)
    value = jnp.zeros(lane.shape, jnp.float32)
    group, offset = divmod(kind * own, LANES)
    for i in range(HD // own):
        piece = joined[head * (HD // own) + i, :, group * LANES : (group + 1) * LANES]
        piece = piece.astype(jnp.float32)
        shift = (i * own - offset) % LANES
        if shift:
            piece = pltpu.roll(piece, shift, 1)
        value = jnp.where((lane >= i * own) & (lane < (i + 1) * own), piece, value)
    return value


def delta_kernel(
    own,
    joined,
    decay_in,
    beta_in,
    scale_ref,
    bias_ref,
    head_gain_ref,
    state_hbm,
    w_out_hbm,
    branch_ref,
    new_hbm,
    state,
    fresh,
    w_out,
    mixed,
    state_sems,
    fresh_sems,
    out_sems,
):
    heads = mixed.shape[0]
    count = state.shape[0]
    width = w_out.shape[1]

    def state_in(h):
        return pltpu.make_async_copy(state_hbm.at[:, h], state.at[:, h], state_sems.at[h])

    def state_out(h):
        return pltpu.make_async_copy(fresh.at[:, h], new_hbm.at[:, h], fresh_sems.at[h])

    for h in range(heads):
        state_in(h).start()
    w_load = pltpu.make_async_copy(w_out_hbm, w_out, out_sems.at[0])
    w_load.start()
    decay = jnp.exp(-scale_ref[...] * jax.nn.softplus(decay_in[...] + bias_ref[...]))
    strength = jax.nn.sigmoid(beta_in[...])
    lane = lax.broadcasted_iota(jnp.int32, decay.shape, 1)

    def one(h, carry):
        query = jax.nn.silu(head_rows(joined, h, 0, own))
        query = (
            query * lax.rsqrt(jnp.sum(query * query, axis=-1, keepdims=True) + EPS) * HD ** (-0.5)
        )
        keys = jax.nn.silu(head_rows(joined, h, 1, own))
        keys = keys * lax.rsqrt(jnp.sum(keys * keys, axis=-1, keepdims=True) + EPS)
        values = jax.nn.silu(head_rows(joined, h, 2, own))
        outgate = jax.nn.silu(head_rows(joined, h, 3, own))
        keep = jnp.sum(jnp.where(lane == h, decay, 0.0), axis=1, keepdims=True)
        beta = jnp.sum(jnp.where(lane == h, strength, 0.0), axis=1, keepdims=True)
        overlap = jnp.sum(keys * query, axis=1, keepdims=True)
        upright = jnp.transpose(jnp.concatenate([keys, query], axis=0))
        state_in(h).wait()
        outputs = []
        for r in range(count):
            held = state[r, h].astype(jnp.float32)
            key = jnp.broadcast_to(upright[:, r : r + 1], held.shape)
            ask = jnp.broadcast_to(upright[:, count + r : count + r + 1], held.shape)
            rate = keep[r : r + 1]
            guess = rate * jnp.sum(key * held, axis=0, keepdims=True)
            change = beta[r : r + 1] * (values[r : r + 1] - guess)
            seen = rate * jnp.sum(ask * held, axis=0, keepdims=True)
            outputs.append(seen + overlap[r : r + 1] * change)
            fresh[r, h] = (rate * held + key * change).astype(jnp.bfloat16)
        state_out(h).start()
        output = rms_scale(jnp.concatenate(outputs, axis=0)) * head_gain_ref[...]
        mixed[h] = (output * outgate).astype(jnp.bfloat16)
        return carry

    lax.fori_loop(0, heads, one, 0)
    w_load.wait()
    rows = jnp.concatenate([mixed[h] for h in range(heads)], axis=1)
    for j in range(0, width, 512):
        branch_ref[:, j : j + 512] = jnp.dot(
            rows, w_out[:, j : j + 512], preferred_element_type=jnp.float32
        )
    for h in range(heads):
        state_out(h).wait()


def delta_part(own, joined, decay_in, beta_in, scale, bias, head_gain, state, w_out):
    count, heads = state.shape[:2]
    vmem = pl.BlockSpec(memory_space=pltpu.VMEM)
    hbm = pl.BlockSpec(memory_space=pltpu.HBM)
    dma = pltpu.SemaphoreType.DMA
    return pl.pallas_call(
        functools.partial(delta_kernel, own),
        out_shape=(
            jax.ShapeDtypeStruct((count, w_out.shape[1]), jnp.float32),
            jax.ShapeDtypeStruct(state.shape, state.dtype),
        ),
        in_specs=[vmem] * 6 + [hbm] * 2,
        out_specs=(vmem, hbm),
        scratch_shapes=[
            pltpu.VMEM(state.shape, state.dtype),
            pltpu.VMEM(state.shape, state.dtype),
            pltpu.VMEM(w_out.shape, w_out.dtype),
            pltpu.VMEM((heads, count, HD), jnp.bfloat16),
            dma((heads,)),
            dma((heads,)),
            dma((1,)),
        ],
        compiler_params=pltpu.CompilerParams(vmem_limit_bytes=VMEM_LIMIT),
    )(joined, decay_in, beta_in, scale[None], bias[None], head_gain[None], state, w_out)


def expert_kernel(
    devices,
    branch_ref,
    shares_ref,
    x_hbm,
    gain_mix_hbm,
    gain_pre_hbm,
    gain_post_hbm,
    gate_hbm,
    up_hbm,
    down_hbm,
    result_ref,
    x_ref,
    gain_mix_ref,
    gain_pre_ref,
    gain_post_ref,
    small_sems,
    buf,
    gate,
    up,
    down,
    hidden,
    weight,
    theirs,
    mine,
    paired,
    total,
    second,
    third,
    fourth,
    gather_send,
    gather_recv,
    load_sems,
    pair_send,
    pair_recv,
    sum_send,
    second_recv,
    third_recv,
    fourth_recv,
):
    place = Place(devices)
    ready = greet(place.partners())
    small = load_all(
        [
            (x_hbm, x_ref),
            (gain_mix_hbm, gain_mix_ref),
            (gain_pre_hbm, gain_pre_ref),
            (gain_post_hbm, gain_post_ref),
        ],
        small_sems,
    )
    loads = load_all([(gate_hbm, gate), (up_hbm, up), (down_hbm, down)], load_sems)
    for load in small:
        load.wait()
    count, width = x_ref.shape
    pieces = gate.shape[1]
    pairs = devices // 2
    x_second = x_ref[...].astype(jnp.float32) + rms_scale(branch_ref[...]) * gain_mix_ref[...]
    buf[place.me] = (rms_scale(x_second) * gain_pre_ref[...]).astype(jnp.bfloat16)
    ready()
    started = gather_blocks(place, buf, gather_send, gather_recv)
    share = shares_ref[:, :, 0:LANES].astype(jnp.float32) + shares_ref[:, :, LANES:].astype(
        jnp.float32
    )
    share = share.reshape(devices * count, LANES)
    lane = lax.broadcasted_iota(jnp.int32, share.shape, 1)
    share = jnp.sum(jnp.where(lane == place.me // PIECES, share, 0.0), axis=1, keepdims=True)
    weight[...] = jnp.broadcast_to(share, (devices * count, LANES)).reshape(weight.shape)
    loads[0].wait()
    loads[1].wait()
    rows = buf[...].reshape(devices * count, width)
    step = 256
    for j in range(0, pieces, step):
        gated = clamped_unit(
            jnp.dot(rows, gate[:, j : j + step], preferred_element_type=jnp.float32),
            jnp.dot(rows, up[:, j : j + step], preferred_element_type=jnp.float32),
        )
        hidden[:, :, :, j : j + step] = gated.astype(jnp.bfloat16).reshape(
            pairs, 2, count, step
        )
    loads[2].wait()

    def parts(core, out):
        units = hidden[:, core].reshape(pairs * count, pieces)
        scale = weight[:, core].reshape(pairs * count, LANES)[:, 0:1]
        for j in range(0, width, 512):
            part = jnp.dot(units, down[:, j : j + 512], preferred_element_type=jnp.float32)
            out[:, :, j : j + 512] = (
                (part * scale).astype(jnp.bfloat16).reshape(pairs, count, 512)
            )

    parts(1 - place.core, theirs)
    sent = []
    for distance in range(place.layers - 1, -1, -1):
        for y, x in ((1, 1), (0, 1), (1, 0), (0, 0)):
            k = place.at(distance, y, x) // 2
            copy = remote(
                theirs.at[k],
                paired.at[k],
                pair_send.at[len(sent)],
                pair_recv.at[k],
                place.at(core=1),
            )
            copy.start()
            sent.append(copy)
    parts(place.core, mine)
    moe, more = reduce_blocks(
        place,
        mine,
        paired,
        total,
        second,
        third,
        fourth,
        (pair_recv, sum_send, second_recv, third_recv, fourth_recv),
    )
    result_ref[...] = (x_second + rms_scale(moe) * gain_post_ref[...]).astype(jnp.bfloat16)
    settle(started + sent + more)


def experts_part(
    devices, branch, x, gain_mix, gain_pre, gain_post, shares, w_gate, w_up, w_down
):
    count, width = x.shape
    layers = devices // 8
    pairs = devices // 2
    pieces = w_gate.shape[1]
    vmem = pl.BlockSpec(memory_space=pltpu.VMEM)
    hbm = pl.BlockSpec(memory_space=pltpu.HBM)
    dma = pltpu.SemaphoreType.DMA

    def blocks(number):
        return pltpu.VMEM((number, count, width), jnp.bfloat16)

    return pl.pallas_call(
        functools.partial(expert_kernel, devices),
        out_shape=jax.ShapeDtypeStruct((count, width), jnp.bfloat16),
        in_specs=[vmem] * 2 + [hbm] * 7,
        out_specs=vmem,
        scratch_shapes=[
            pltpu.VMEM(x.shape, x.dtype),
            pltpu.VMEM((1, width), jnp.float32),
            pltpu.VMEM((1, width), jnp.float32),
            pltpu.VMEM((1, width), jnp.float32),
            dma((4,)),
            blocks(devices),
            pltpu.VMEM(w_gate.shape, jnp.bfloat16),
            pltpu.VMEM(w_up.shape, jnp.bfloat16),
            pltpu.VMEM(w_down.shape, jnp.bfloat16),
            pltpu.VMEM((pairs, 2, count, pieces), jnp.bfloat16),
            pltpu.VMEM((pairs, 2, count, LANES), jnp.float32),
            blocks(pairs),
            blocks(pairs),
            blocks(pairs),
            blocks(pairs),
            blocks(2 * layers),
            blocks(layers),
            blocks(layers),
            dma((gather_sends(devices),)),
            dma((devices,)),
            dma((3,)),
            dma((pairs,)),
            dma((pairs,)),
            dma((4 * layers,)),
            dma((2 * layers,)),
            dma((layers,)),
            dma((layers,)),
        ],
        compiler_params=pltpu.CompilerParams(
            collective_id=1, has_side_effects=True, vmem_limit_bytes=VMEM_LIMIT
        ),
    )(
        branch,
        shares,
        x,
        gain_mix[None],
        gain_pre[None],
        gain_post[None],
        w_gate,
        w_up,
        w_down,
    )


def shards(
    residual_in,
    gain_mix_pre,
    w_query,
    w_key,
    w_value,
    w_outgate,
    w_decay,
    w_beta,
    decay_scale,
    decay_bias,
    head_gain,
    w_out,
    gain_mix_post,
    state_cache,
    gain_ffn_pre,
    routes,
    route_logits,
    w_gate,
    w_up,
    w_down,
    gain_ffn_post,
):
    devices = lax.axis_size("ep")
    joined, shares, decay_in, beta_in = project(
        devices,
        residual_in,
        gain_mix_pre,
        routes,
        route_logits,
        w_query,
        w_key,
        w_value,
        w_outgate,
        w_decay,
        w_beta,
    )
    branch, new_state = delta_part(
        w_query.shape[1],
        joined,
        decay_in,
        beta_in,
        decay_scale,
        decay_bias,
        head_gain,
        state_cache,
        w_out,
    )
    result = experts_part(
        devices,
        branch,
        residual_in,
        gain_mix_post,
        gain_ffn_pre,
        gain_ffn_post,
        shares,
        w_gate,
        w_up,
        w_down,
    )
    return (result, new_state)


def solution(mesh):
    in_specs = (
        P("ep", None),
        P(),
        P(None, "ep"),
        P(None, "ep"),
        P(None, "ep"),
        P(None, "ep"),
        P(),
        P(),
        P(),
        P(),
        P(),
        P(),
        P(),
        P("ep", None, None, None),
        P(),
        P("ep", None),
        P("ep", None),
        P(None, "ep"),
        P(None, "ep"),
        P("ep", None),
        P(),
    )
    out_specs = (P("ep", None), P("ep", None, None, None))
    return jax.shard_map(shards, mesh=mesh, in_specs=in_specs, out_specs=out_specs, check_vma=False)
```
